32 devices in a mesh: ep: 8 (over z, x), tp: 4 (over y, core).
Axes of the slice: x: 2, y: 2, z: 4, core: 2. Of those that a mesh axis runs over, the one named last changes fastest.
Arguments:
- queries: bfloat16 [2048, 1024], P('ep', 'tp'), may hold values from -256 to 256
- key_rows: bfloat16 [2048, 1024], P('ep', 'tp'), may hold values from -8 to 8
- value_rows: bfloat16 [2048, 1024], P('ep', 'tp'), may hold values from -6 to 6
- head_lambda: float32 [8], P('tp'), may hold values from 0.3 to 0.8
- sub_gain: float32 [128], replicated, may hold values from 0.1 to 1.9
- out_weight: bfloat16 [1024, 2048], P('tp'), may hold values from -0.1875 to 0.1875
- expert_input: bfloat16 [1536, 2048], P('ep'), may hold values from -6 to 6
- norm_gain: float32 [2048], replicated, may hold values from 0.1 to 1.9
- route_ids: int32 [1536, 2], P('ep'), may hold values from 0 to 7, all different within a row; in each aligned block of 192 rows (0 to 191, 192 to 383, ...) at most 80 rows name the same one
- route_weight: float32 [1536, 2], P('ep'), may hold values from 0.25 to 1
- gate_weight: bfloat16 [8, 2048, 3584], P('ep', None, 'tp'), may hold values from -0.125 to 0.125
- up_weight: bfloat16 [8, 2048, 3584], P('ep', None, 'tp'), may hold values from -0.125 to 0.125
- down_weight: bfloat16 [8, 3584, 2048], P('ep', 'tp'), may hold values from -0.09375 to 0.09375
Outputs:
- mixer_out: bfloat16 [2048, 2048], P(('ep', 'tp'))
- expert_out: bfloat16 [1536, 2048], P('ep', 'tp')
The draws below stay inside these ranges and needn't reach their ends.
Inputs may be any that keep to these rules, and one draw needn't show every extreme that they name: `route_ids`: each row names 2 different experts. In each aligned block of 192 rows no expert is named by more than 80 rows, a bound that some block reaches.
All inputs are finite; a program needn't handle non-finite values.
Results may differ from the reference program's by a relative error of at most 0.014.
Values may be sent and summed in bfloat16 or wider, within the bound.
A program may use at most 256 MiB of HBM per device.

```python
import math
import jax
import jax.numpy as jnp
import numpy as np
from jax import lax

D = 2048
HEADS = 8
HEAD_DIM = 64
VALUE_DIM = 128
FF = 3584
TOP = 2
TOK_B_DEV = 192
EXPERTS = 8
CAP = 80
TOKENS_A = 2048
TOKENS_B = 1536
N_EP = 8
N_TP = 4


def query_key_pair(key):
    base = jax.random.fold_in(key, 11)
    key_draw, query_draw = jax.random.split(base, 2)
    shape = (TOKENS_A, HEADS, 2, HEAD_DIM)
    key_vals = 1.3 * jax.random.truncated_normal(key_draw, -6.0, 6.0, shape, jnp.float32)
    query_vals = 1.3 * jax.random.truncated_normal(query_draw, -6.0, 6.0, shape, jnp.float32)
    return (query_vals.reshape(TOKENS_A, HEADS * 2 * HEAD_DIM), key_vals.reshape(TOKENS_A, HEADS * 2 * HEAD_DIM))


def draw_queries(key, part):
    return query_key_pair(key)[0].astype(jnp.bfloat16)


def draw_key_rows(key, part):
    return query_key_pair(key)[1].astype(jnp.bfloat16)


def block_scale(stream_key, dims, cuts, smallest, largest):
    loudness, own = 1.0, jax.random.fold_in(stream_key, 6)
    for position, parts in cuts:
        draws = jnp.exp(jax.random.uniform(jax.random.fold_in(own, position), (parts,), jnp.float32, smallest / len(cuts), largest / len(cuts)))
        loudness = loudness * jnp.repeat(draws, dims[position] // parts).reshape([-1 if axis == position else 1 for axis in range(len(dims))])
    return loudness


def shared_out(stream_key, own, number, rows, count, top, limit, skew):
    order = jax.random.permutation(stream_key, count)
    heavy_load, usual = portions_of(count, rows * top, limit, skew, True), portions_of(count, rows * top, limit, skew, False)
    places = jnp.arange(count)

    def named(lengths, offset_by):
        used = int((lengths > 0).sum())
        fixed = max(1, used // 4)
        passed = fixed + (places - fixed + offset_by * (used - fixed)) % max(1, count - fixed)
        return jnp.zeros((count,), jnp.int32).at[order[jnp.where(places < fixed, places, passed)]].set(jnp.asarray(lengths, jnp.int32))

    lengths = jnp.where(number % 4 == 0, named(heavy_load, number // 4), named(usual, number - number // 4 - 1))
    mixed = jax.random.permutation(jax.random.fold_in(own, 3), count)
    source_of, receiver = mixed[0:count // 2 * 2:2], mixed[1:count // 2 * 2:2]
    slack = jnp.minimum(lengths[source_of] - 1, limit - lengths[receiver]) // 2
    slack = jnp.where((source_of == order[0]) | (receiver == order[0]) | (lengths[receiver] == 0), 0, jnp.maximum(slack, 0))
    passed = jax.random.randint(jax.random.fold_in(own, 4), (count // 2,), 0, 1 << 20) % (slack + 1)
    lengths = lengths.at[source_of].add(-passed).at[receiver].add(passed)
    items = jnp.searchsorted(jnp.cumsum(lengths), jnp.arange(rows * top), side="right").astype(jnp.int32)
    grid = items.reshape(top, rows).T
    grid = grid[jax.random.permutation(jax.random.fold_in(own, 1), rows)]
    offset_by = jax.random.randint(jax.random.fold_in(own, 2), (rows, 1), 0, top)
    return jnp.take_along_axis(grid, (jnp.arange(top)[None, :] + offset_by) % top, axis=1)


def portions_of(amount, total, limit, skew, full):
    loads = [(1 << 20) // math.isqrt(standing ** skew) + 1 for standing in range(1, amount + 1)]
    largest = limit if full else min(limit, max(-(-total // amount), total * loads[0] // sum(loads)))
    least = 1 if total - largest >= amount - 1 else 0
    holding, rest = [largest] + [least] * (amount - 1), total - largest - least * (amount - 1)
    while rest > 0:
        free = [i for i in range(1, amount) if holding[i] < largest] or [i for i in range(1, amount) if holding[i] < limit]
        whole, budget = sum([loads[i] for i in free]), rest
        for i in free:
            addition = min(limit - holding[i], max(1, budget * loads[i] // whole), rest)
            holding[i] = holding[i] + addition
            rest = rest - addition
    return np.array(holding)


def noise(key, shape, spread, reach, shards=(), kind=jnp.bfloat16):
    level = block_scale(key, shape, shards, -0.22, 0.18) if shards else 1.0
    entries = jax.random.normal(key, shape, jnp.float32) * spread * level
    return jnp.minimum(jnp.maximum(entries, -reach), reach).astype(kind)


def setup_inputs(seed: int = 0) -> dict:
    arg_keys = jax.random.split(jax.random.key(seed), 14)
    queries = draw_queries(jax.random.fold_in(arg_keys[13], 71), 0)
    key_rows = draw_key_rows(jax.random.fold_in(arg_keys[13], 71), 0)
    value_rows = noise(arg_keys[2], (TOKENS_A, HEADS * VALUE_DIM), 1.0, 6.0, ((0, 8), (1, 4)))
    head_lambda = jnp.clip(0.3 + 0.5 * jax.random.uniform(arg_keys[3], (HEADS,), jnp.float32) ** block_scale(arg_keys[3], (HEADS,), ((0, 4),), -0.2, 0.2), 0.3, 0.8)
    sub_gain = jnp.clip(1.0 + 0.18 * jax.random.normal(arg_keys[4], (VALUE_DIM,), jnp.float32), 0.1, 1.9)
    out_weight = noise(arg_keys[5], (HEADS * VALUE_DIM, D), (HEADS * VALUE_DIM) ** -0.5, 0.1875, ((0, 4),))
    expert_input = noise(arg_keys[6], (TOKENS_B, D), 1.0, 6.0, ((0, 8),))
    norm_gain = jnp.clip(1.0 + 0.18 * jax.random.normal(arg_keys[7], (D,), jnp.float32), 0.1, 1.9)
    route_ids_keys = jax.random.split(jax.random.fold_in(arg_keys[8], 1), TOKENS_B // TOK_B_DEV)
    route_ids_turns = jax.random.permutation(jax.random.fold_in(arg_keys[8], 3), TOKENS_B // TOK_B_DEV)
    route_ids = jax.vmap(lambda own, number: shared_out(jax.random.fold_in(arg_keys[8], 2), own, number, TOK_B_DEV, EXPERTS, TOP, CAP, 1))(route_ids_keys, route_ids_turns).reshape((TOKENS_B, TOP))
    route_weight = jnp.clip(0.25 + 0.75 * jax.random.uniform(arg_keys[9], (TOKENS_B, TOP), jnp.float32) ** block_scale(arg_keys[9], (TOKENS_B, TOP), ((0, 8),), -0.2, 0.2), 0.25, 1.0)
    gate_weight = noise(arg_keys[10], (EXPERTS, D, FF), D ** -0.5, 0.125, ((0, 8), (2, 4)))
    up_weight = noise(arg_keys[11], (EXPERTS, D, FF), D ** -0.5, 0.125, ((0, 8), (2, 4)))
    down_weight = noise(arg_keys[12], (EXPERTS, FF, D), FF ** -0.5, 0.09375, ((0, 8), (1, 4)))
    return {"queries": queries, "key_rows": key_rows, "value_rows": value_rows, "head_lambda": head_lambda, "sub_gain": sub_gain, "out_weight": out_weight, "expert_input": expert_input, "norm_gain": norm_gain, "route_ids": route_ids, "route_weight": route_weight, "gate_weight": gate_weight, "up_weight": up_weight, "down_weight": down_weight}


EPS = 1e-06

def round_keep(values):
    return lax.optimization_barrier(values.astype(jnp.bfloat16)).astype(jnp.float32)

def head_output(query_head, key_head, value_head, lam_value, sub_gain):
    block_rows = math.gcd(TOKENS_A, 512)
    scaling = HEAD_DIM ** (-0.5)
    key_pos = jnp.arange(TOKENS_A, dtype=jnp.int32)
    key_wide = key_head.astype(jnp.float32)
    value_wide = value_head.astype(jnp.float32)

    def one_block(block_index):
        first_row = (block_index * block_rows).astype(jnp.int32)
        query_block = lax.dynamic_slice_in_dim(query_head, first_row, block_rows, 0).astype(jnp.float32)
        scores = jnp.einsum('qmd,kmd->mqk', query_block, key_wide) * scaling
        query_pos = first_row + jnp.arange(block_rows, dtype=jnp.int32)
        allowed = query_pos[:, None] >= key_pos[None, :]
        scores = jnp.where(allowed, scores, -jnp.inf)
        row_max = lax.optimization_barrier(jnp.max(scores, axis=-1, keepdims=True))
        weights = jnp.where(allowed, jnp.exp(scores - row_max), 0.0)
        row_total = lax.optimization_barrier(jnp.sum(weights, axis=-1))
        numerator = jnp.einsum('mqk,kd->mqd', round_keep(weights), value_wide)
        per_map = numerator / row_total[..., None]
        contrast = per_map[0] - lam_value * per_map[1]
        normed = contrast * lax.rsqrt(lax.optimization_barrier(jnp.mean(contrast * contrast, axis=-1, keepdims=True)) + EPS) * sub_gain
        return normed.astype(jnp.bfloat16)
    blocks = lax.map(one_block, jnp.arange(TOKENS_A // block_rows, dtype=jnp.int32))
    return blocks.reshape(TOKENS_A, VALUE_DIM)

def reference(queries, key_rows, value_rows, head_lambda, sub_gain, out_weight, expert_input, norm_gain, route_ids, route_weight, gate_weight, up_weight, down_weight):
    query_heads = jnp.moveaxis(queries.reshape(TOKENS_A, HEADS, 2, HEAD_DIM), 1, 0)
    key_heads = jnp.moveaxis(key_rows.reshape(TOKENS_A, HEADS, 2, HEAD_DIM), 1, 0)
    value_heads = jnp.moveaxis(value_rows.reshape(TOKENS_A, HEADS, VALUE_DIM), 1, 0)

    def per_head(operands):
        return head_output(operands[0], operands[1], operands[2], operands[3], sub_gain)
    attended = lax.map(per_head, (query_heads, key_heads, value_heads, head_lambda))
    attended = jnp.moveaxis(attended, 0, 1).reshape(TOKENS_A, HEADS * VALUE_DIM)
    group_cols = HEADS // N_TP * VALUE_DIM
    mixed_sum = jnp.zeros((TOKENS_A, D), jnp.float32)
    for group_index in range(N_TP):
        lower = group_index * group_cols
        share = jnp.dot(attended[:, lower:lower + group_cols], out_weight[lower:lower + group_cols], preferred_element_type=jnp.float32)
        mixed_sum = mixed_sum + round_keep(share)
    mixer_out = mixed_sum.astype(jnp.bfloat16)
    wide_rows = expert_input.astype(jnp.float32)
    normed_input = (wide_rows * lax.rsqrt(lax.optimization_barrier(jnp.mean(wide_rows * wide_rows, axis=-1, keepdims=True)) + EPS) * norm_gain).astype(jnp.bfloat16)
    flat_ids = route_ids.reshape(N_EP, TOK_B_DEV * TOP)
    onehot = (flat_ids[..., None] == jnp.arange(EXPERTS, dtype=jnp.int32)).astype(jnp.int32)
    rank_before = jnp.cumsum(onehot, axis=1) - onehot
    slot_index = lax.optimization_barrier(jnp.sum(rank_before * onehot, axis=-1))
    source = jnp.arange(N_EP, dtype=jnp.int32)[:, None]
    buffer_pos = ((flat_ids * N_EP + source) * CAP + slot_index).astype(jnp.int32)
    token_index = (source * TOK_B_DEV + jnp.arange(TOK_B_DEV * TOP, dtype=jnp.int32)[None, :] // TOP).astype(jnp.int32)
    row_table = jnp.full((EXPERTS * N_EP * CAP,), TOKENS_B, jnp.int32)
    row_table = row_table.at[buffer_pos.reshape(-1)].set(token_index.reshape(-1))
    padded = jnp.concatenate([normed_input, jnp.zeros((1, D), jnp.bfloat16)], axis=0)
    unit_share = FF // N_TP

    def one_expert(operands):
        gathered = padded[operands[0]]
        gate_act = jnp.dot(gathered, operands[1], preferred_element_type=jnp.float32)
        up_act = jnp.dot(gathered, operands[2], preferred_element_type=jnp.float32)
        hidden = (jax.nn.silu(gate_act) * up_act).astype(jnp.bfloat16)
        result_sum = jnp.zeros((N_EP * CAP, D), jnp.float32)
        for group_index in range(N_TP):
            lower = group_index * unit_share
            share = jnp.dot(hidden[:, lower:lower + unit_share], operands[3][lower:lower + unit_share], preferred_element_type=jnp.float32)
            result_sum = result_sum + round_keep(share)
        return result_sum.astype(jnp.bfloat16)
    results = lax.map(one_expert, (row_table.reshape(EXPERTS, N_EP * CAP), gate_weight, up_weight, down_weight))
    picked = results.reshape(EXPERTS * N_EP * CAP, D)[buffer_pos.reshape(-1)]
    picked = picked.reshape(TOKENS_B, TOP, D).astype(jnp.float32)
    expert_out = lax.optimization_barrier(jnp.sum(picked * route_weight[..., None], axis=1)).astype(jnp.bfloat16)
    return (mixer_out, expert_out)
```

```python
import functools

import jax
import jax.numpy as jnp
from jax import lax
from jax.experimental import pallas as pl
from jax.experimental.pallas import tpu as pltpu
from jax.sharding import PartitionSpec as P

EPS = 1e-06
MESH = pl.DeviceIdType.MESH
F32 = jnp.float32
BF16 = jnp.bfloat16


def flip(index, bits):
    low = 1
    while low <= bits:
        if bits & low:
            index = index + low - 2 * low * ((index // low) % 2)
        low *= 2
    return index


def dot(a, b, dims=((1,), (0,)), precision=None):
    return lax.dot_general(a, b, (dims, ((), ())), precision=precision, preferred_element_type=F32)


def kernel(
    n_ep, cap, lam, q, k, v, gain, x, norm_gain, ids, route_w, wo_hbm, wg_hbm, wu_hbm, wd_hbm,
    mixer, expert,
    wo, wg, wu, wd, arr, hidden, part, sib, ysend, yrecv, res, ret, kbuf, vbuf,
    outb, qs, comb, acc, top, tot, att, hp, hsib, hysend, hyrecv,
    w_sem, d_send, d_recv, f_send, f_recv, r_send, r_recv, s_send, s_recv, y_send, y_recv,
    kv_send, kv_recv, h_send, h_recv,
):
    me = lax.axis_index("ep")
    tp = lax.axis_index("tp")
    half = n_ep // 2
    tokens, width = x.shape
    cols = width // 4
    units = wg.shape[1]
    core = tp % 2
    sib_tp, y_tp = flip(tp, 1), flip(tp, 2)

    def remote(src, dst, ssem, rsem, where):
        return pltpu.make_async_remote_copy(
            src_ref=src, dst_ref=dst, send_sem=ssem, recv_sem=rsem,
            device_id=where, device_id_type=MESH,
        )

    weights = [
        pltpu.make_async_copy(a, b, w_sem.at[i])
        for i, (a, b) in enumerate(((wg_hbm, wg), (wu_hbm, wu), (wd_hbm, wd), (wo_hbm, wo)))
    ]
    for copy in weights:
        copy.start()

    barrier = pltpu.get_barrier_semaphore()
    for d in range(1, n_ep):
        pl.semaphore_signal(barrier, inc=1, device_id=(flip(me, d), tp), device_id_type=MESH)
    for d in range(1, 4):
        pl.semaphore_signal(barrier, inc=1, device_id=(me, flip(tp, d)), device_id_type=MESH)

    lane = lax.broadcasted_iota(jnp.int32, (tokens, 128), 1)
    id0, id1 = ids[:, 0:1], ids[:, 1:2]
    hot0, hot1 = (lane == id0).astype(F32), (lane == id1).astype(F32)
    earlier = (
        lax.broadcasted_iota(jnp.int32, (tokens, tokens), 1)
        < lax.broadcasted_iota(jnp.int32, (tokens, tokens), 0)
    ).astype(F32).astype(BF16)
    rank = dot(earlier, (hot0 + hot1).astype(BF16))
    pos0 = (id0 * cap).astype(F32) + jnp.sum(rank * hot0, axis=1, keepdims=True)
    pos1 = (id1 * cap).astype(F32) + jnp.sum(rank * hot1, axis=1, keepdims=True)
    packed = jnp.where(lane == 0, pos0, jnp.where(lane == 1, pos1, 0.0))
    pick = (
        lax.broadcasted_iota(jnp.int32, (8, 128), 0) == lax.broadcasted_iota(jnp.int32, (8, 128), 1)
    ).astype(F32)
    pos_rows = dot(pick, packed, ((1,), (1,)), lax.Precision.HIGHEST)
    row0 = (pos_rows[0:1] + 0.5).astype(jnp.int32)
    row1 = (pos_rows[1:2] + 0.5).astype(jnp.int32)
    slots = n_ep * cap
    slot = lax.broadcasted_iota(jnp.int32, (slots, tokens), 0)
    dispatch = ((slot == row0) | (slot == row1)).astype(F32).astype(BF16)
    wide = x[...].astype(F32)
    inv = lax.rsqrt(jnp.mean(wide * wide, axis=-1, keepdims=True) + EPS)
    mine = pl.ds(pl.multiple_of(tp * cols, cols), cols)
    normed = (x[:, mine].astype(F32) * inv * norm_gain[:, mine]).astype(BF16)
    outb[...] = dot(dispatch, normed).astype(BF16).reshape(n_ep, cap, cols)
    slot_c = lax.broadcasted_iota(jnp.int32, (tokens, slots), 1)
    comb[...] = jnp.where(slot_c == pos0.astype(jnp.int32), route_w[:, 0:1], 0.0) + jnp.where(
        slot_c == pos1.astype(jnp.int32), route_w[:, 1:2], 0.0
    )
    arr[tp, me] = outb[me]
    kbuf[me] = k[...]
    vbuf[me] = v[...]
    pl.semaphore_wait(barrier, n_ep - 1 + 3)

    sends = {}
    for d in range(1, n_ep):
        to = flip(me, d)
        sends[d] = remote(
            outb.at[to], arr.at[tp, me], d_send.at[d], d_recv.at[d], (to, tp)
        )
        sends[d].start()

    pending = [[], []]
    relays = [[], []]

    def forward(group):
        for d in range(group * half, (group + 1) * half):
            src = flip(me, d)
            if d:
                sends[d].wait_recv()
            for j, to in ((0, sib_tp), (1, y_tp)):
                c = remote(arr.at[tp, src], arr.at[tp, src], f_send.at[j, d], f_recv.at[j, d], (me, to))
                c.start()
                pending[group].append((j, c))

    def relay(group):
        first = [c for j, c in pending[group] if j == 1]
        for i, d in enumerate(range(group * half, (group + 1) * half)):
            first[i].wait_recv()
            src = flip(me, d)
            c = remote(
                arr.at[y_tp, src], arr.at[y_tp, src], f_send.at[2, d], f_recv.at[2, d], (me, sib_tp)
            )
            c.start()
            relays[group].append(c)

    def arrived(group):
        for j, c in pending[group]:
            if j == 0:
                c.wait_recv()
        for c in relays[group]:
            c.wait_recv()

    mine_half = me // half
    rows = half * cap

    def base_of(group):
        return (mine_half + group * (1 - 2 * mine_half)) * half

    def gate_up(group):
        base = base_of(group)

        def step(i, carry):
            at = pl.ds(pl.multiple_of(i * 128, 128), 128)
            total = jnp.zeros((rows, 256), F32)
            for t in range(4):
                w = jnp.concatenate(
                    [wg[t * cols:(t + 1) * cols, at], wu[t * cols:(t + 1) * cols, at]], axis=1
                )
                total += dot(arr[t, pl.ds(base, half)].reshape(rows, cols), w)
            g, u = total[:, :128], total[:, 128:]
            hidden[:, at] = (g / (1.0 + jnp.exp(-g)) * u).astype(BF16)
            return carry

        lax.fori_loop(0, units // 128, step, 0)

    def down(group):
        base = base_of(group)
        for t in range(4):
            def step(i, carry):
                at = pl.multiple_of(i * 256, 256)
                out = dot(hidden[...], wd[:, pl.ds(t * cols + at, 256)])
                part[t, pl.ds(base, half), :, pl.ds(at, 256)] = out.astype(BF16).reshape(half, cap, 256)
                return carry

            lax.fori_loop(0, cols // 256, step, 0)

    def pair_sum(group):
        base = base_of(group)
        copies = []
        for y in range(2):
            c = remote(
                part.at[2 * y + 1 - core, pl.ds(base, half)], sib.at[y, pl.ds(base, half)],
                s_send.at[group, y], s_recv.at[group, y], (me, sib_tp),
            )
            c.start()
            copies.append(c)
        return copies

    my_y = tp // 2

    def y_sum(group, copies):
        base = base_of(group)
        at = pl.ds(base, half)
        for c in copies:
            c.wait()
        ysend[at] = (part[y_tp, at].astype(F32) + sib[1 - my_y, at].astype(F32)).astype(BF16)
        c = remote(ysend.at[at], yrecv.at[at], y_send.at[group], y_recv.at[group], (me, y_tp))
        c.start()
        return c

    def give_back(group, copy):
        base = base_of(group)
        at = pl.ds(base, half)
        copy.wait()
        res[at] = (
            part[tp, at].astype(F32) + sib[my_y, at].astype(F32) + yrecv[at].astype(F32)
        ).astype(BF16)
        out = []
        for d in range(group * half, (group + 1) * half):
            if d:
                to = flip(me, d)
                c = remote(res.at[to], ret.at[me], r_send.at[d], r_recv.at[d], (to, tp))
                c.start()
                out.append(c)
            else:
                ret[me] = res[me]
        return out

    across = flip(me, 1)
    level, side = me // 2, me % 2
    levels = n_ep // 2

    def kv_copy(b, way, up):
        buf = kbuf if b == 0 else vbuf
        def make(block):
            to = lax.rem(me + 2, n_ep) if up else across
            idx = block // 2
            return remote(
                buf.at[block], buf.at[block], kv_send.at[way, b, idx], kv_recv.at[way, b, idx], (to, tp)
            )
        return make

    def kv_send_block(lev):
        block = 2 * lev + side

        @pl.when(level < levels - 1)
        def _():
            for b in range(2):
                kv_copy(b, 0, True)(block).start()

        @pl.when((lev < level) | (side == 0))
        def _():
            for b in range(2):
                kv_copy(b, 1, False)(block).start()

    def kv_hop(step):
        @pl.when(level - step >= 0)
        def _():
            lev = level - step
            for b in range(2):
                kv_copy(b, 0, True)(2 * lev + side).wait_recv()
            kv_send_block(lev)

    def kv_across(lev):
        block = 2 * lev + 1 - side
        for b in range(2):
            kv_copy(b, 1, False)(block).wait_recv()

    def kv_finish():
        def step(lev, carry):
            block = 2 * lev + side

            @pl.when(level < levels - 1)
            def _():
                for b in range(2):
                    kv_copy(b, 0, True)(block).wait_send()

            @pl.when((lev < level) | (side == 0))
            def _():
                for b in range(2):
                    kv_copy(b, 1, False)(block).wait_send()

            return carry

        lax.fori_loop(0, level + 1, step, 0)

    q_rows = q.shape[0]
    heads = lam.shape[0]
    pair = q.shape[1] // heads
    head_width = pair // 2
    head_lane = lax.broadcasted_iota(jnp.int32, (q_rows, pair), 1)

    def attend_own():
        for h in range(heads):
            at = slice(h * pair, (h + 1) * pair)
            qh = q[:, at].astype(F32) * (head_width ** -0.5)
            qs[h, :q_rows] = jnp.where(head_lane < head_width, qh, 0.0).astype(BF16)
            qs[h, q_rows:] = jnp.where(head_lane < head_width, 0.0, qh).astype(BF16)
            s = dot(qs[h], k[:, at], ((1,), (1,)))
            qp = lax.broadcasted_iota(jnp.int32, s.shape, 0) % q_rows
            ok = qp >= lax.broadcasted_iota(jnp.int32, s.shape, 1)
            s = jnp.where(ok, s, -1e30)
            m = jnp.max(s, axis=1, keepdims=True)
            w = jnp.where(ok, jnp.exp(s - m), 0.0)
            top[h] = m
            tot[h] = jnp.sum(w, axis=1, keepdims=True)
            acc[h] = dot(w.astype(BF16), v[:, at])

    def attend(block):
        kb, vb = kbuf.at[block], vbuf.at[block]
        for h in range(heads):
            at = slice(h * pair, (h + 1) * pair)
            s = dot(qs[h], kb[:, at], ((1,), (1,)))
            old = top[h]
            m = jnp.maximum(old, jnp.max(s, axis=1, keepdims=True))
            scale = jnp.exp(old - m)
            w = jnp.exp(s - m)
            top[h] = m
            tot[h] = tot[h] * scale + jnp.sum(w, axis=1, keepdims=True)
            acc[h] = acc[h] * scale + dot(w.astype(BF16), vb[:, at])

    def attend_rest():
        def step(i, carry):
            lev = level - i

            @pl.when(i > 0)
            def _():
                attend(2 * lev + side)

            @pl.when((i > 0) | (side == 1))
            def _():
                kv_across(lev)
                attend(2 * lev + 1 - side)

            return carry

        lax.fori_loop(0, level + 1, step, 0)

    def project():
        outs = []
        for h in range(heads):
            a = acc[h] / tot[h]
            contrast = a[:q_rows] - lam[h] * a[q_rows:]
            norm = lax.rsqrt(jnp.mean(contrast * contrast, axis=-1, keepdims=True) + EPS)
            outs.append((contrast * norm * gain[...]).astype(BF16))
        att[...] = jnp.concatenate(outs, axis=1)

        def step(i, carry):
            at = pl.ds(pl.multiple_of(i * 256, 256), 256)
            hp[:, :, at] = dot(att[...], wo[:, at]).astype(BF16).reshape(4, q_rows // 4, 256)
            return carry

        lax.fori_loop(0, width // 256, step, 0)
        copies = []
        for y in range(2):
            c = remote(
                hp.at[2 * y + 1 - core], hsib.at[y], h_send.at[y], h_recv.at[y], (me, sib_tp)
            )
            c.start()
            copies.append(c)
        return copies

    forward(0)
    relay(0)
    forward(1)
    kv_send_block(level)
    weights[0].wait()
    weights[1].wait()
    arrived(0)
    gate_up(0)
    relay(1)
    weights[2].wait()
    down(0)
    pair0 = pair_sum(0)
    kv_hop(1)
    arrived(1)
    gate_up(1)
    y0 = y_sum(0, pair0)
    for step in range(2, min(levels, 3)):
        kv_hop(step)
    down(1)
    pair1 = pair_sum(1)
    for step in range(3, levels):
        kv_hop(step)
    attend_own()
    back = give_back(0, y0)
    y1 = y_sum(1, pair1)
    attend_rest()
    back += give_back(1, y1)
    weights[3].wait()
    hcopies = project()
    for c in hcopies:
        c.wait()
    hysend[...] = (hp[y_tp].astype(F32) + hsib[1 - my_y].astype(F32)).astype(BF16)
    hy = remote(hysend, hyrecv, h_send.at[2], h_recv.at[2], (me, y_tp))
    hy.start()
    for d in range(1, n_ep):
        sends[d].wait_send()
    for group in range(2):
        for j, c in pending[group]:
            c.wait_send()
        for c in relays[group]:
            c.wait_send()
    kv_finish()
    hy.wait()
    mixer[...] = (hp[tp].astype(F32) + hsib[my_y].astype(F32) + hyrecv[...].astype(F32)).astype(BF16)
    for c in back:
        c.wait()
    big = comb[...]
    high = big.astype(BF16)
    low = (big - high.astype(F32)).astype(BF16)
    got = ret[...].reshape(slots, cols)
    expert[...] = (dot(high, got) + dot(low, got)).astype(BF16)


def solution(mesh):
    n_ep = mesh.shape["ep"]

    def shards(
        queries, key_rows, value_rows, head_lambda, sub_gain, out_weight, expert_input, norm_gain,
        route_ids, route_weight, gate_weight, up_weight, down_weight,
    ):
        tokens, width = expert_input.shape
        cap = 5 * route_ids.shape[1] * tokens // (3 * n_ep)
        cap = -(-cap // 16) * 16
        cols = width // 4
        half = n_ep // 2
        units = gate_weight.shape[2]
        q_rows, kv_cols = queries.shape
        heads = head_lambda.shape[0]
        vm = pl.BlockSpec(memory_space=pltpu.VMEM)
        hbm = pl.BlockSpec(memory_space=pl.ANY)
        dma = pltpu.SemaphoreType.DMA
        return pl.pallas_call(
            functools.partial(kernel, n_ep, cap),
            name="both_halves",
            out_shape=(
                jax.ShapeDtypeStruct((q_rows // 4, width), BF16),
                jax.ShapeDtypeStruct((tokens, cols), BF16),
            ),
            in_specs=[pl.BlockSpec(memory_space=pltpu.SMEM)] + [vm] * 8 + [hbm] * 4,
            out_specs=(vm, vm),
            scratch_shapes=[
                pltpu.VMEM(out_weight.shape, BF16),
                pltpu.VMEM((width, units), BF16),
                pltpu.VMEM((width, units), BF16),
                pltpu.VMEM((units, width), BF16),
                pltpu.VMEM((4, n_ep, cap, cols), BF16),
                pltpu.VMEM((half * cap, units), BF16),
                pltpu.VMEM((4, n_ep, cap, cols), BF16),
                pltpu.VMEM((2, n_ep, cap, cols), BF16),
                pltpu.VMEM((n_ep, cap, cols), BF16),
                pltpu.VMEM((n_ep, cap, cols), BF16),
                pltpu.VMEM((n_ep, cap, cols), BF16),
                pltpu.VMEM((n_ep, cap, cols), BF16),
                pltpu.VMEM((n_ep, q_rows, kv_cols), BF16),
                pltpu.VMEM((n_ep, q_rows, kv_cols), BF16),
                pltpu.VMEM((n_ep, cap, cols), BF16),
                pltpu.VMEM((heads, 2 * q_rows, 128), BF16),
                pltpu.VMEM((tokens, n_ep * cap), F32),
                pltpu.VMEM((heads, 2 * q_rows, 128), F32),
                pltpu.VMEM((heads, 2 * q_rows, 1), F32),
                pltpu.VMEM((heads, 2 * q_rows, 1), F32),
                pltpu.VMEM((q_rows, kv_cols), BF16),
                pltpu.VMEM((4, q_rows // 4, width), BF16),
                pltpu.VMEM((2, q_rows // 4, width), BF16),
                pltpu.VMEM((q_rows // 4, width), BF16),
                pltpu.VMEM((q_rows // 4, width), BF16),
                dma((4,)),
                dma((n_ep,)), dma((n_ep,)),
                dma((3, n_ep)), dma((3, n_ep)),
                dma((n_ep,)), dma((n_ep,)),
                dma((2, 2)), dma((2, 2)),
                dma((2,)), dma((2,)),
                dma((2, 2, half)), dma((2, 2, half)),
                dma((3,)), dma((3,)),
            ],
            compiler_params=pltpu.CompilerParams(
                collective_id=0, has_side_effects=True, vmem_limit_bytes=62 * 1024 * 1024
            ),
        )(
            head_lambda, queries, key_rows, value_rows, sub_gain.reshape(1, -1), expert_input,
            norm_gain.reshape(1, -1), route_ids, route_weight, out_weight,
            gate_weight[0], up_weight[0], down_weight[0],
        )

    placed = (
        P("ep", "tp"), P("ep", "tp"), P("ep", "tp"), P("tp"), P(), P("tp", None), P("ep", None), P(),
        P("ep", None), P("ep", None), P("ep", None, "tp"), P("ep", None, "tp"), P("ep", "tp", None),
    )
    return jax.shard_map(
        shards, mesh=mesh, in_specs=placed,
        out_specs=(P(("ep", "tp"), None), P("ep", "tp")), check_vma=False,
    )
```

```python
import functools

import jax
import jax.numpy as jnp
from jax import lax
from jax.experimental import pallas as pl
from jax.experimental.pallas import tpu as pltpu
from jax.sharding import PartitionSpec as P

EPS = 1e-06
MESH = pl.DeviceIdType.MESH
F32 = jnp.float32
BF16 = jnp.bfloat16


def flip(index, bits):
    low = 1
    while low <= bits:
        if bits & low:
            index = index + low - 2 * low * ((index // low) % 2)
        low *= 2
    return index


def dot(a, b, dims=((1,), (0,)), precision=None):
    return lax.dot_general(a, b, (dims, ((), ())), precision=precision, preferred_element_type=F32)


def kernel(
    n_ep, cap, lam, q, k, v, gain, x, norm_gain, ids, route_w, wo_hbm, wg_hbm, wu_hbm, wd_hbm,
    mixer, expert,
    wo, wg, wu, wd, arr, hidden, part, sib, ysend, yrecv, res, ret, kbuf, vbuf,
    outb, qs, comb, acc, top, att, hp, hsib, hysend, hyrecv,
    w_sem, d_send, d_recv, f_send, f_recv, r_send, r_recv, s_send, s_recv, y_send, y_recv,
    kv_send, kv_recv, h_send, h_recv,
):
    me = lax.axis_index("ep")
    tp = lax.axis_index("tp")
    half = n_ep // 2
    tokens, width = x.shape
    cols = width // 4
    units = wg.shape[1]
    core = tp % 2
    sib_tp, y_tp = flip(tp, 1), flip(tp, 2)

    def remote(src, dst, ssem, rsem, where):
        return pltpu.make_async_remote_copy(
            src_ref=src, dst_ref=dst, send_sem=ssem, recv_sem=rsem,
            device_id=where, device_id_type=MESH,
        )

    weights = [
        pltpu.make_async_copy(a, b, w_sem.at[i])
        for i, (a, b) in enumerate(((wg_hbm, wg), (wu_hbm, wu), (wd_hbm, wd), (wo_hbm, wo)))
    ]
    for copy in weights:
        copy.start()

    barrier = pltpu.get_barrier_semaphore()
    for d in range(1, n_ep):
        pl.semaphore_signal(barrier, inc=1, device_id=(flip(me, d), tp), device_id_type=MESH)
    for d in range(1, 4):
        pl.semaphore_signal(barrier, inc=1, device_id=(me, flip(tp, d)), device_id_type=MESH)

    lane = lax.broadcasted_iota(jnp.int32, (tokens, 128), 1)
    id0, id1 = ids[:, 0:1], ids[:, 1:2]
    hot0, hot1 = (lane == id0).astype(F32), (lane == id1).astype(F32)
    earlier = (
        lax.broadcasted_iota(jnp.int32, (tokens, tokens), 1)
        < lax.broadcasted_iota(jnp.int32, (tokens, tokens), 0)
    ).astype(F32).astype(BF16)
    rank = dot(earlier, (hot0 + hot1).astype(BF16))
    pos0 = (id0 * cap).astype(F32) + jnp.sum(rank * hot0, axis=1, keepdims=True)
    pos1 = (id1 * cap).astype(F32) + jnp.sum(rank * hot1, axis=1, keepdims=True)
    packed = jnp.where(lane == 0, pos0, jnp.where(lane == 1, pos1, 0.0))
    pick = (
        lax.broadcasted_iota(jnp.int32, (8, 128), 0) == lax.broadcasted_iota(jnp.int32, (8, 128), 1)
    ).astype(F32)
    pos_rows = dot(pick, packed, ((1,), (1,)), lax.Precision.HIGHEST)
    row0 = (pos_rows[0:1] + 0.5).astype(jnp.int32)
    row1 = (pos_rows[1:2] + 0.5).astype(jnp.int32)
    slots = n_ep * cap
    slot = lax.broadcasted_iota(jnp.int32, (slots, tokens), 0)
    dispatch = ((slot == row0) | (slot == row1)).astype(F32).astype(BF16)
    wide = x[...].astype(F32)
    inv = lax.rsqrt(jnp.mean(wide * wide, axis=-1, keepdims=True) + EPS)
    mine = pl.ds(pl.multiple_of(tp * cols, cols), cols)
    normed = (x[:, mine].astype(F32) * inv * norm_gain[:, mine]).astype(BF16)
    outb[...] = dot(dispatch, normed).astype(BF16).reshape(n_ep, cap, cols)
    slot_c = lax.broadcasted_iota(jnp.int32, (tokens, slots), 1)
    comb[...] = jnp.where(slot_c == pos0.astype(jnp.int32), route_w[:, 0:1], 0.0) + jnp.where(
        slot_c == pos1.astype(jnp.int32), route_w[:, 1:2], 0.0
    )
    arr[tp, me] = outb[me]
    kbuf[me] = k[...]
    vbuf[me] = v[...]
    pl.semaphore_wait(barrier, n_ep - 1 + 3)

    sends = {}
    for d in range(1, n_ep):
        to = flip(me, d)
        sends[d] = remote(
            outb.at[to], arr.at[tp, me], d_send.at[d], d_recv.at[d], (to, tp)
        )
        sends[d].start()

    pending = [[], []]
    relays = [[], []]

    def forward(group):
        for d in range(group * half, (group + 1) * half):
            src = flip(me, d)
            if d:
                sends[d].wait_recv()
            for j, to in ((0, sib_tp), (1, y_tp)):
                c = remote(arr.at[tp, src], arr.at[tp, src], f_send.at[j, d], f_recv.at[j, d], (me, to))
                c.start()
                pending[group].append((j, c))

    def relay(group):
        first = [c for j, c in pending[group] if j == 1]
        for i, d in enumerate(range(group * half, (group + 1) * half)):
            first[i].wait_recv()
            src = flip(me, d)
            c = remote(
                arr.at[y_tp, src], arr.at[y_tp, src], f_send.at[2, d], f_recv.at[2, d], (me, sib_tp)
            )
            c.start()
            relays[group].append(c)

    def arrived(group):
        for j, c in pending[group]:
            if j == 0:
                c.wait_recv()
        for c in relays[group]:
            c.wait_recv()

    mine_half = me // half
    rows = half * cap

    def base_of(group):
        return (mine_half + group * (1 - 2 * mine_half)) * half

    def gate_up(group):
        base = base_of(group)

        def step(i, carry):
            at = pl.ds(pl.multiple_of(i * 128, 128), 128)
            total = jnp.zeros((rows, 256), F32)
            for t in range(4):
                w = jnp.concatenate(
                    [wg[t * cols:(t + 1) * cols, at], wu[t * cols:(t + 1) * cols, at]], axis=1
                )
                total += dot(arr[t, pl.ds(base, half)].reshape(rows, cols), w)
            g, u = total[:, :128], total[:, 128:]
            hidden[:, at] = (g / (1.0 + jnp.exp(-g)) * u).astype(BF16)
            return carry

        lax.fori_loop(0, units // 128, step, 0)

    def down(group):
        base = base_of(group)
        for t in range(4):
            def step(i, carry):
                at = pl.multiple_of(i * 256, 256)
                out = dot(hidden[...], wd[:, pl.ds(t * cols + at, 256)])
                part[t, pl.ds(base, half), :, pl.ds(at, 256)] = out.astype(BF16).reshape(half, cap, 256)
                return carry

            lax.fori_loop(0, cols // 256, step, 0)

    def pair_sum(group):
        base = base_of(group)
        copies = []
        for y in range(2):
            c = remote(
                part.at[2 * y + 1 - core, pl.ds(base, half)], sib.at[y, pl.ds(base, half)],
                s_send.at[group, y], s_recv.at[group, y], (me, sib_tp),
            )
            c.start()
            copies.append(c)
        return copies

    my_y = tp // 2

    def y_sum(group, copies):
        base = base_of(group)
        at = pl.ds(base, half)
        for c in copies:
            c.wait()
        ysend[at] = (part[y_tp, at].astype(F32) + sib[1 - my_y, at].astype(F32)).astype(BF16)
        c = remote(ysend.at[at], yrecv.at[at], y_send.at[group], y_recv.at[group], (me, y_tp))
        c.start()
        return c

    def give_back(group, copy):
        base = base_of(group)
        at = pl.ds(base, half)
        copy.wait()
        res[at] = (
            part[tp, at].astype(F32) + sib[my_y, at].astype(F32) + yrecv[at].astype(F32)
        ).astype(BF16)
        out = []
        for d in range(group * half, (group + 1) * half):
            if d:
                to = flip(me, d)
                c = remote(res.at[to], ret.at[me], r_send.at[d], r_recv.at[d], (to, tp))
                c.start()
                out.append(c)
            else:
                ret[me] = res[me]
        return out

    across = flip(me, 1)
    level, side = me // 2, me % 2
    levels = n_ep // 2

    def kv_copy(b, way, up):
        buf = kbuf if b == 0 else vbuf
        def make(block):
            to = lax.rem(me + 2, n_ep) if up else across
            idx = block // 2
            return remote(
                buf.at[block], buf.at[block], kv_send.at[way, b, idx], kv_recv.at[way, b, idx], (to, tp)
            )
        return make

    def kv_up(lev):
        block = 2 * lev + side

        @pl.when(level < levels - 1)
        def _():
            for b in range(2):
                kv_copy(b, 0, True)(block).start()

    def kv_over(lev):
        block = 2 * lev + side

        @pl.when((lev < level) | (side == 0))
        def _():
            for b in range(2):
                kv_copy(b, 1, False)(block).start()

    def kv_hop(step):
        @pl.when(level - step >= 0)
        def _():
            lev = level - step
            for b in range(2):
                kv_copy(b, 0, True)(2 * lev + side).wait_recv()
            kv_up(lev)
            kv_over(lev)

    def kv_across(lev):
        block = 2 * lev + 1 - side
        for b in range(2):
            kv_copy(b, 1, False)(block).wait_recv()

    def kv_finish():
        def step(lev, carry):
            block = 2 * lev + side

            @pl.when(level < levels - 1)
            def _():
                for b in range(2):
                    kv_copy(b, 0, True)(block).wait_send()

            @pl.when((lev < level) | (side == 0))
            def _():
                for b in range(2):
                    kv_copy(b, 1, False)(block).wait_send()

            return carry

        lax.fori_loop(0, level + 1, step, 0)

    q_rows = q.shape[0]
    heads = lam.shape[0]
    pair = q.shape[1] // heads
    head_width = pair // 2
    head_lane = lax.broadcasted_iota(jnp.int32, (q_rows, pair), 1)

    def attend_own():
        for h in range(heads):
            at = slice(h * pair, (h + 1) * pair)
            qh = q[:, at].astype(F32) * (head_width ** -0.5)
            qs[h, :q_rows] = jnp.where(head_lane < head_width, qh, 0.0).astype(BF16)
            qs[h, q_rows:] = jnp.where(head_lane < head_width, 0.0, qh).astype(BF16)
            s = dot(qs[h], k[:, at], ((1,), (1,)))
            qp = lax.broadcasted_iota(jnp.int32, s.shape, 0) % q_rows
            ok = qp >= lax.broadcasted_iota(jnp.int32, s.shape, 1)
            s = jnp.where(ok, s, -1e30)
            m = jnp.max(s, axis=1, keepdims=True)
            w = jnp.where(ok, jnp.exp(s - m), 0.0)
            top[h] = m
            acc[h] = dot(w.astype(BF16), with_ones(v[:, at]))

    def with_ones(vb):
        return jnp.concatenate([vb, jnp.ones(vb.shape, BF16)], axis=1)

    def attend(first, count):
        span = pl.ds(first, count)
        for h in range(heads):
            at = slice(h * pair, (h + 1) * pair)
            kb = kbuf[span, :, at].reshape(count * q_rows, pair)
            vb = vbuf[span, :, at].reshape(count * q_rows, pair)
            s = dot(qs[h], kb, ((1,), (1,)))
            old = top[h]
            m = jnp.maximum(old, jnp.max(s, axis=1, keepdims=True))
            w = jnp.exp(s - m)
            top[h] = m
            acc[h] = acc[h] * jnp.exp(old - m) + dot(w.astype(BF16), with_ones(vb))

    def attend_level():
        @pl.when(side == 1)
        def _():
            kv_across(level)
            attend(2 * level, 1)

    def attend_rest(lo, hi):
        def step(i, carry):
            kv_across(level - i)
            attend(2 * (level - i), 2)
            return carry

        lax.fori_loop(lo, jnp.minimum(hi, level + 1), step, 0)

    def project():
        outs = []
        for h in range(heads):
            a = acc[h, :, :pair] / acc[h, :, pair:]
            contrast = a[:q_rows] - lam[h] * a[q_rows:]
            norm = lax.rsqrt(jnp.mean(contrast * contrast, axis=-1, keepdims=True) + EPS)
            outs.append((contrast * norm * gain[...]).astype(BF16))
        att[...] = jnp.concatenate(outs, axis=1)

        def step(i, carry):
            at = pl.ds(pl.multiple_of(i * 256, 256), 256)
            hp[:, :, at] = dot(att[...], wo[:, at]).astype(BF16).reshape(4, q_rows // 4, 256)
            return carry

        lax.fori_loop(0, width // 256, step, 0)
        copies = []
        for y in range(2):
            c = remote(
                hp.at[2 * y + 1 - core], hsib.at[y], h_send.at[y], h_recv.at[y], (me, sib_tp)
            )
            c.start()
            copies.append(c)
        return copies

    kv_over(level)
    attend_own()
    forward(0)
    relay(0)
    forward(1)
    kv_up(level)
    weights[0].wait()
    weights[1].wait()
    arrived(0)
    gate_up(0)
    relay(1)
    weights[2].wait()
    down(0)
    pair0 = pair_sum(0)
    kv_hop(1)
    arrived(1)
    gate_up(1)
    y0 = y_sum(0, pair0)
    for step in range(2, min(levels, 3)):
        kv_hop(step)
    down(1)
    pair1 = pair_sum(1)
    for step in range(3, levels):
        kv_hop(step)
    back = give_back(0, y0)
    attend_level()
    y1 = y_sum(1, pair1)
    attend_rest(1, 2)
    back += give_back(1, y1)
    attend_rest(2, levels)
    weights[3].wait()
    hcopies = project()
    for c in hcopies:
        c.wait()
    hysend[...] = (hp[y_tp].astype(F32) + hsib[1 - my_y].astype(F32)).astype(BF16)
    hy = remote(hysend, hyrecv, h_send.at[2], h_recv.at[2], (me, y_tp))
    hy.start()
    for d in range(1, n_ep):
        sends[d].wait_send()
    for group in range(2):
        for j, c in pending[group]:
            c.wait_send()
        for c in relays[group]:
            c.wait_send()
    kv_finish()
    hy.wait()
    mixer[...] = (hp[tp].astype(F32) + hsib[my_y].astype(F32) + hyrecv[...].astype(F32)).astype(BF16)
    for c in back:
        c.wait()
    big = comb[...]
    high = big.astype(BF16)
    low = (big - high.astype(F32)).astype(BF16)
    got = ret[...].reshape(slots, cols)
    expert[...] = (dot(high, got) + dot(low, got)).astype(BF16)


def solution(mesh):
    n_ep = mesh.shape["ep"]

    def shards(
        queries, key_rows, value_rows, head_lambda, sub_gain, out_weight, expert_input, norm_gain,
        route_ids, route_weight, gate_weight, up_weight, down_weight,
    ):
        tokens, width = expert_input.shape
        cap = 5 * route_ids.shape[1] * tokens // (3 * n_ep)
        cap = -(-cap // 16) * 16
        cols = width // 4
        half = n_ep // 2
        units = gate_weight.shape[2]
        q_rows, kv_cols = queries.shape
        heads = head_lambda.shape[0]
        vm = pl.BlockSpec(memory_space=pltpu.VMEM)
        hbm = pl.BlockSpec(memory_space=pl.ANY)
        dma = pltpu.SemaphoreType.DMA
        return pl.pallas_call(
            functools.partial(kernel, n_ep, cap),
            name="both_halves",
            out_shape=(
                jax.ShapeDtypeStruct((q_rows // 4, width), BF16),
                jax.ShapeDtypeStruct((tokens, cols), BF16),
            ),
            in_specs=[pl.BlockSpec(memory_space=pltpu.SMEM)] + [vm] * 8 + [hbm] * 4,
            out_specs=(vm, vm),
            scratch_shapes=[
                pltpu.VMEM(out_weight.shape, BF16),
                pltpu.VMEM((width, units), BF16),
                pltpu.VMEM((width, units), BF16),
                pltpu.VMEM((units, width), BF16),
                pltpu.VMEM((4, n_ep, cap, cols), BF16),
                pltpu.VMEM((half * cap, units), BF16),
                pltpu.VMEM((4, n_ep, cap, cols), BF16),
                pltpu.VMEM((2, n_ep, cap, cols), BF16),
                pltpu.VMEM((n_ep, cap, cols), BF16),
                pltpu.VMEM((n_ep, cap, cols), BF16),
                pltpu.VMEM((n_ep, cap, cols), BF16),
                pltpu.VMEM((n_ep, cap, cols), BF16),
                pltpu.VMEM((n_ep, q_rows, kv_cols), BF16),
                pltpu.VMEM((n_ep, q_rows, kv_cols), BF16),
                pltpu.VMEM((n_ep, cap, cols), BF16),
                pltpu.VMEM((heads, 2 * q_rows, 128), BF16),
                pltpu.VMEM((tokens, n_ep * cap), F32),
                pltpu.VMEM((heads, 2 * q_rows, 2 * kv_cols // heads), F32),
                pltpu.VMEM((heads, 2 * q_rows, 1), F32),
                pltpu.VMEM((q_rows, kv_cols), BF16),
                pltpu.VMEM((4, q_rows // 4, width), BF16),
                pltpu.VMEM((2, q_rows // 4, width), BF16),
                pltpu.VMEM((q_rows // 4, width), BF16),
                pltpu.VMEM((q_rows // 4, width), BF16),
                dma((4,)),
                dma((n_ep,)), dma((n_ep,)),
                dma((3, n_ep)), dma((3, n_ep)),
                dma((n_ep,)), dma((n_ep,)),
                dma((2, 2)), dma((2, 2)),
                dma((2,)), dma((2,)),
                dma((2, 2, half)), dma((2, 2, half)),
                dma((3,)), dma((3,)),
            ],
            compiler_params=pltpu.CompilerParams(
                collective_id=0, has_side_effects=True, vmem_limit_bytes=62 * 1024 * 1024
            ),
        )(
            head_lambda, queries, key_rows, value_rows, sub_gain.reshape(1, -1), expert_input,
            norm_gain.reshape(1, -1), route_ids, route_weight, out_weight,
            gate_weight[0], up_weight[0], down_weight[0],
        )

    placed = (
        P("ep", "tp"), P("ep", "tp"), P("ep", "tp"), P("tp"), P(), P("tp", None), P("ep", None), P(),
        P("ep", None), P("ep", None), P("ep", None, "tp"), P("ep", None, "tp"), P("ep", "tp", None),
    )
    return jax.shard_map(
        shards, mesh=mesh, in_specs=placed,
        out_specs=(P(("ep", "tp"), None), P("ep", "tp")), check_vma=False,
    )
```
